32 devices in a mesh: sp: 8 (over z, x), tp: 4 (over y, core).
Axes of the slice: x: 2, y: 2, z: 4, core: 2. Of those that a mesh axis runs over, the one named last changes fastest.
Arguments:
- mid: bfloat16 [1536, 2048], P('sp'), may hold values from -6 to 6
- out_grad: bfloat16 [1536, 2048], P('sp'), may hold values from -6 to 6
- expert_ids: int32 [1536, 2], P('sp'), may hold values from 0 to 7, all different within a row; in each aligned block of 192 rows (0 to 191, 192 to 383, ...) at most 72 rows name the same one
- route_weights: float32 [1536, 2], P('sp'), may hold values from 0.1 to 0.9
- gate_proj: bfloat16 [8, 2048, 1024], P('sp', None, 'tp'), may hold values from -0.375 to 0.375
- up_proj: bfloat16 [8, 2048, 1024], P('sp', None, 'tp'), may hold values from -0.375 to 0.375
- down_proj: bfloat16 [8, 1024, 2048], P('sp', 'tp'), may hold values from -0.1875 to 0.1875
- out_proj: bfloat16 [512, 2048], P('tp'), may hold values from -0.25 to 0.25
- branch_gate: bfloat16 [1536, 512], P('sp', 'tp'), may hold values from -6 to 6
- conv_out: bfloat16 [2, 1536, 512], P(None, 'sp', 'tp'), may hold values from -6 to 6
- prior_state: float32 [2, 1536, 512], P(None, 'sp', 'tp'), may hold values from -6 to 6
- rate_gate_w: bfloat16 [2, 8, 64, 64], P(None, 'tp'), may hold values from -0.75 to 0.75
- input_gate_w: bfloat16 [2, 8, 64, 64], P(None, 'tp'), may hold values from -0.75 to 0.75
- decay_param: float32 [2, 512], P(None, 'tp'), may hold values from 4 to 16
- decay_jump: float32 [2, 1536, 512], P(None, 'sp', 'tp'), may hold values from -2 to 0
- conv_taps: bfloat16 [2, 4, 512], P(None, None, 'tp'), may hold values from -3 to 3
Outputs:
- gate_grad: bfloat16 [8, 2048, 1024], P('sp', None, 'tp')
- up_grad: bfloat16 [8, 2048, 1024], P('sp', None, 'tp')
- down_grad: bfloat16 [8, 1024, 2048], P('sp', 'tp')
- proj_grad_t: float32 [2048, 512], P('sp', 'tp')
- input_grad: bfloat16 [1536, 512], P('sp', 'tp')
- branch_gate_grad: bfloat16 [1536, 512], P('sp', 'tp')
The draws below stay inside these ranges and needn't reach their ends.
Inputs may be any that keep to these rules, and one draw needn't show every extreme that they name: `expert_ids`: each row names 2 different experts. Among the rows of one device no expert is named by more than 72 rows, a bound that some block reaches of some device.
All inputs are finite; a program needn't handle non-finite values.
Results may differ from the reference program's by a relative error of at most 0.023.
The reference program's roundings to bfloat16 on the way count: a program that leaves them out, or rounds other values in their place, can miss the bound.
Values may be sent and summed in bfloat16 or wider, within the bound.
A program may use at most 64 MiB of HBM per device.

```python
import math
import jax
import jax.numpy as jnp
import numpy as np
from jax import lax

D = 2048
FF = 1024
HEADS = 8
HEAD = 64
W = 512
TAPS = 4
TOP = 2
EXPERTS = 8
TOK_DEV = 192
CAP = 72
STREAM_ITEMS = 1536
N_SP = 8
N_TP = 4


def draw_decay_param(key, part):
    selection_seed, slow_key, fast_key = jax.random.split(jax.random.fold_in(key, 11), 3)
    slow_share = 0.5
    slow_mask = jax.random.uniform(selection_seed, (2, W), jnp.float32) < slow_share
    slow_rate = jnp.exp(jax.random.uniform(slow_key, (2, W), jnp.float32, jnp.log(0.02), jnp.log(0.12))) / STREAM_ITEMS
    fast_rate = jnp.exp(jax.random.uniform(fast_key, (2, W), jnp.float32, jnp.log(0.0025), jnp.log(0.008)))
    rates = jnp.where(slow_mask, slow_rate, fast_rate)
    return -jnp.log(jnp.expm1(rates))


def draw_decay_jump(key, part):
    block_key, place_key, loss_key = jax.random.split(jax.random.fold_in(key, 23), 3)
    block_count = STREAM_ITEMS // TOK_DEV
    factors = jnp.exp(jax.random.uniform(block_key, (2, block_count, 1), jnp.float32, jnp.log(0.1), jnp.log(0.8)))
    equilibrium_level = -jnp.repeat(factors, TOK_DEV, axis=1) / STREAM_ITEMS
    assigned_positions = jax.random.randint(place_key, (2, 2), 0, STREAM_ITEMS)
    objective_scores = jax.random.uniform(loss_key, (2, 2, W), jnp.float32, 0.2, 0.5)
    arrival_tallies = (jnp.arange(STREAM_ITEMS, dtype=jnp.int32)[None, :, None] == assigned_positions[:, None, :]).astype(jnp.float32)
    return equilibrium_level + jnp.einsum('dwp,dpu->dwu', arrival_tallies, jnp.log1p(-objective_scores))


def spiked(drawn, key, source, target, parts, factor):
    owner, partner = [(jnp.arange(drawn.shape[axis_at]) // (drawn.shape[axis_at] // parts)).reshape([-1 if axis == axis_at else 1 for axis in range(drawn.ndim)]) for axis_at in (source, target)]
    chosen = jax.random.permutation(key, parts)[partner]
    strong = (owner == chosen) | (owner == (partner + parts // 2) % parts)
    return jnp.where(strong, factor * drawn, drawn)


def steps_of(key, extent, cuts, least, top_value):
    def one(axis_at, blocks):
        draws = jax.random.uniform(jax.random.fold_in(jax.random.fold_in(key, 6), axis_at), (blocks,), jnp.float32, least / len(cuts), top_value / len(cuts))
        return jnp.repeat(jnp.exp(draws), extent[axis_at] // blocks).reshape((-1,) + (1,) * (len(extent) - axis_at - 1))

    loudness = one(*cuts[0])
    for cut in cuts[1:]:
        loudness = loudness * one(*cut)
    return loudness


def routed_block(stream_key, own, number, rows, count, top, limit, slope):
    ranking = jax.random.permutation(stream_key, count)
    packed, usual = shares(count, rows * top, limit, slope, True), shares(count, rows * top, limit, slope, False)
    places = jnp.arange(count)

    def named(tallies, turn):
        used = int((tallies > 0).sum())
        fixed = max(1, used // 4)
        shifted = fixed + (places - fixed + turn * (used - fixed)) % max(1, count - fixed)
        return jnp.zeros((count,), jnp.int32).at[ranking[jnp.where(places < fixed, places, shifted)]].set(jnp.asarray(tallies, jnp.int32))

    tallies = jnp.where(number % 4 == 0, named(packed, number // 4), named(usual, number - number // 4 - 1))
    mixed = jax.random.permutation(jax.random.fold_in(own, 3), count)
    giver, sink = mixed[0:count // 2 * 2:2], mixed[1:count // 2 * 2:2]
    slack = jnp.minimum(tallies[giver] - 1, limit - tallies[sink]) // 2
    slack = jnp.where((giver == ranking[0]) | (sink == ranking[0]) | (tallies[sink] == 0), 0, jnp.maximum(slack, 0))
    shifted = jax.random.randint(jax.random.fold_in(own, 4), (count // 2,), 0, 1 << 20) % (slack + 1)
    tallies = tallies.at[giver].add(-shifted).at[sink].add(shifted)
    labels = jnp.searchsorted(jnp.cumsum(tallies), jnp.arange(rows * top), side="right").astype(jnp.int32)
    listing = labels.reshape(top, rows).T
    listing = listing[jax.random.permutation(jax.random.fold_in(own, 1), rows)]
    turn = jax.random.randint(jax.random.fold_in(own, 2), (rows, 1), 0, top)
    return jnp.take_along_axis(listing, (jnp.arange(top)[None, :] + turn) % top, axis=1)


def shares(number_of, total, bound, skew, full):
    weights = [(1 << 20) // math.isqrt(rank ** skew) + 1 for rank in range(1, number_of + 1)]
    largest = bound if full else min(bound, max(-(-total // number_of), total * weights[0] // sum(weights)))
    least = 1 if total - largest >= number_of - 1 else 0
    given, surplus = [largest] + [least] * (number_of - 1), total - largest - least * (number_of - 1)
    while surplus > 0:
        candidates = [i for i in range(1, number_of) if given[i] < largest] or [i for i in range(1, number_of) if given[i] < bound]
        pool, left = sum([weights[i] for i in candidates]), surplus
        for i in candidates:
            more = min(bound - given[i], max(1, left * weights[i] // pool), surplus)
            given[i] = given[i] + more
            surplus = surplus - more
    return np.array(given)


def normal_values(rng, extent, width, most, shards=(), held_as=jnp.bfloat16):
    loudness = steps_of(rng, extent, shards, -0.22, 0.18) if shards else 1.0
    entries = jax.random.normal(rng, extent, jnp.float32) * width * loudness
    return jnp.minimum(jnp.maximum(entries, -most), most).astype(held_as)


def heavy_noise(rng, dims, width, most, cuts, heavy, kind=jnp.bfloat16):
    values = width * jax.random.normal(rng, dims, jnp.float32)
    if cuts:
        values = values * steps_of(rng, dims, cuts, -0.22, 0.18)
    return jnp.clip(spiked(values, jax.random.fold_in(rng, 3), *heavy), -most, most).astype(kind)


def setup_inputs(seed: int = 0) -> dict:
    keys = jax.random.split(jax.random.key(seed), 17)
    mid = normal_values(keys[0], (STREAM_ITEMS, D), 1.0, 6.0, ((0, 8),))
    out_grad = heavy_noise(keys[1], (STREAM_ITEMS, D), 1.0, 6.0, ((0, 8),), (0, 1, 8, 2.0))
    expert_ids_keys = jax.random.split(jax.random.fold_in(keys[2], 1), STREAM_ITEMS // TOK_DEV)
    expert_ids_turns = jax.random.permutation(jax.random.fold_in(keys[2], 3), STREAM_ITEMS // TOK_DEV)
    expert_ids = jax.vmap(lambda own, number: routed_block(jax.random.fold_in(keys[2], 2), own, number, TOK_DEV, EXPERTS, TOP, CAP, 1))(expert_ids_keys, expert_ids_turns).reshape((STREAM_ITEMS, TOP))
    route_weights = jnp.clip(0.1 + 0.79999997 * jax.random.uniform(keys[3], (STREAM_ITEMS, TOP), jnp.float32) ** steps_of(keys[3], (STREAM_ITEMS, TOP), ((0, 8),), -0.2, 0.2), 0.1, 0.9)
    gate_proj = normal_values(keys[4], (EXPERTS, D, FF), (D // 9) ** -0.5, 0.375, ((0, 8), (2, 4)))
    up_proj = normal_values(keys[5], (EXPERTS, D, FF), (D // 9) ** -0.5, 0.375, ((0, 8), (2, 4)))
    down_proj = normal_values(keys[6], (EXPERTS, FF, D), FF ** -0.5, 0.1875, ((0, 8), (1, 4)))
    out_proj = normal_values(keys[7], (W, D), W ** -0.5, 0.25, ((0, 4),))
    branch_gate = normal_values(keys[8], (STREAM_ITEMS, W), 1.0, 6.0, ((0, 8), (1, 4)))
    conv_out = normal_values(keys[9], (2, STREAM_ITEMS, W), 1.0, 6.0, ((1, 8), (2, 4)))
    prior_state = normal_values(keys[10], (2, STREAM_ITEMS, W), 1.0, 6.0, ((1, 8), (2, 4)), jnp.float32)
    rate_gate_w = normal_values(keys[11], (2, HEADS, HEAD, HEAD), HEAD ** -0.5, 0.75, ((1, 4),))
    input_gate_w = normal_values(keys[12], (2, HEADS, HEAD, HEAD), HEAD ** -0.5, 0.75, ((1, 4),))
    decay_param = draw_decay_param(jax.random.fold_in(keys[16], 71), 0)
    decay_jump = draw_decay_jump(jax.random.fold_in(keys[16], 71), 0)
    conv_taps = normal_values(keys[15], (2, TAPS, W), 0.5, 3.0, ((2, 4),))
    return {"mid": mid, "out_grad": out_grad, "expert_ids": expert_ids, "route_weights": route_weights, "gate_proj": gate_proj, "up_proj": up_proj, "down_proj": down_proj, "out_proj": out_proj, "branch_gate": branch_gate, "conv_out": conv_out, "prior_state": prior_state, "rate_gate_w": rate_gate_w, "input_gate_w": input_gate_w, "decay_param": decay_param, "decay_jump": decay_jump, "conv_taps": conv_taps}


RATE_SCALE = 8.0
CLAMP_LIMIT = 7.0
SHARPNESS = 1.702
NORM_EPSILON = 1e-06
STATE_FLOOR = 0.001
GELU_CUBIC = 0.044715
GELU_SCALE = 0.7978845608028654

def gelu_parts(values):
    inside = GELU_SCALE * (values + GELU_CUBIC * values * values * values)
    tangent = jnp.tanh(inside)
    result = 0.5 * values * (1.0 + tangent)
    slope_value = 0.5 * (1.0 + tangent) + 0.5 * values * (1.0 - tangent * tangent) * GELU_SCALE * (1.0 + 3.0 * GELU_CUBIC * values * values)
    return (result, slope_value)

def adjoint_chain(decay_factors, seeds, backward):

    def advance(incoming, step_pair):
        adjoint_now = step_pair[1] + incoming
        return (step_pair[0] * adjoint_now, adjoint_now)
    start_carry = jnp.zeros(seeds.shape[1:], jnp.float32)
    _, totals = lax.scan(advance, start_carry, (decay_factors, seeds), reverse=backward)
    return totals

def reference(mid, out_grad, expert_ids, route_weights, gate_proj, up_proj, down_proj, out_proj, branch_gate, conv_out, prior_state, rate_gate_w, input_gate_w, decay_param, decay_jump, conv_taps):
    mid_full = mid.astype(jnp.float32)
    inv_rms = lax.rsqrt(lax.optimization_barrier(jnp.mean(mid_full * mid_full, axis=1, keepdims=True)) + NORM_EPSILON)
    normed = mid_full * inv_rms
    normed_b = normed.astype(jnp.bfloat16)
    block_ids = expert_ids.reshape(N_SP, TOK_DEV * TOP)
    onehot = (block_ids[:, :, None] == jnp.arange(EXPERTS, dtype=jnp.int32)[None, None, :]).astype(jnp.int32)
    rank_ids = lax.optimization_barrier(jnp.sum((jnp.cumsum(onehot, axis=1) - onehot) * onehot, axis=2))
    positions = (jnp.arange(N_SP, dtype=jnp.int32)[:, None] * CAP + rank_ids).reshape(-1)
    flat_ids = expert_ids.reshape(-1)
    slot_table = jnp.full((EXPERTS, N_SP * CAP), -1, jnp.int32).at[flat_ids, positions].set(jnp.arange(STREAM_ITEMS * TOP, dtype=jnp.int32))
    route_flat = route_weights.reshape(-1)
    ff_group = FF // N_TP

    def expert_step(running, inputs):
        slot_rows, w_gate, w_up, down_weight = inputs
        filled = slot_rows >= 0
        assign = jnp.where(filled, slot_rows, 0)
        token_ids = assign // TOP
        rows_b = jnp.where(filled[:, None], normed_b[token_ids], jnp.zeros((), jnp.bfloat16))
        weights = jnp.where(filled, route_flat[assign], 0.0)
        grad_b = (out_grad[token_ids].astype(jnp.float32) * weights[:, None]).astype(jnp.bfloat16)
        gate_pre = jnp.dot(rows_b, w_gate, preferred_element_type=jnp.float32)
        up_pre = jnp.dot(rows_b, w_up, preferred_element_type=jnp.float32)
        gate_clamped = jnp.minimum(gate_pre, CLAMP_LIMIT)
        up_clamped = jnp.clip(up_pre, -CLAMP_LIMIT, CLAMP_LIMIT)
        gate_sigmoid = jax.nn.sigmoid(SHARPNESS * gate_clamped)
        swish_value = gate_clamped * gate_sigmoid
        act_b = ((up_clamped + 1.0) * swish_value).astype(jnp.bfloat16)
        act_grad = jnp.dot(grad_b, down_weight.T, preferred_element_type=jnp.float32)
        gate_delta = jnp.where(gate_pre < CLAMP_LIMIT, act_grad * (up_clamped + 1.0) * (gate_sigmoid + SHARPNESS * swish_value * (1.0 - gate_sigmoid)), 0.0).astype(jnp.bfloat16)
        up_delta = jnp.where(jnp.abs(up_pre) < CLAMP_LIMIT, act_grad * swish_value, 0.0).astype(jnp.bfloat16)
        down_grad = jnp.dot(act_b.T, grad_b, preferred_element_type=jnp.float32).astype(jnp.bfloat16)
        gate_grad = jnp.dot(rows_b.T, gate_delta, preferred_element_type=jnp.float32).astype(jnp.bfloat16)
        up_grad = jnp.dot(rows_b.T, up_delta, preferred_element_type=jnp.float32).astype(jnp.bfloat16)
        gate_parts = gate_delta.astype(jnp.float32).reshape(-1, N_TP, ff_group)
        up_parts = up_delta.astype(jnp.float32).reshape(-1, N_TP, ff_group)
        gate_cols = w_gate.astype(jnp.float32).reshape(D, N_TP, ff_group)
        up_cols = w_up.astype(jnp.float32).reshape(D, N_TP, ff_group)
        partials = jnp.einsum('rjf,djf->jrd', gate_parts, gate_cols) + jnp.einsum('rjf,djf->jrd', up_parts, up_cols)
        rounded = lax.optimization_barrier(partials.astype(jnp.bfloat16))
        slot_b = lax.optimization_barrier(jnp.sum(rounded.astype(jnp.float32), axis=0)).astype(jnp.bfloat16)
        running = running.at[token_ids].add(jnp.where(filled[:, None], slot_b.astype(jnp.float32), 0.0))
        return (running, (gate_grad, up_grad, down_grad))
    token_grad, (gate_grads, up_grads, down_grads) = lax.scan(expert_step, jnp.zeros((STREAM_ITEMS, D), jnp.float32), (slot_table, gate_proj, up_proj, down_proj))
    inner_mean = lax.optimization_barrier(jnp.mean(token_grad * normed, axis=1, keepdims=True))
    mid_grad_b = (out_grad.astype(jnp.float32) + inv_rms * (token_grad - normed * inner_mean)).astype(jnp.bfloat16)
    branch_grad = jnp.dot(mid_grad_b, out_proj.T, preferred_element_type=jnp.float32)
    conv_full = conv_out.astype(jnp.float32)
    conv_heads = conv_full.reshape(2, STREAM_ITEMS, HEADS, HEAD)
    rate_gate = jax.nn.sigmoid(jnp.einsum('sthc,shcd->sthd', conv_heads, rate_gate_w.astype(jnp.float32)).reshape(2, STREAM_ITEMS, W))
    input_gate = jax.nn.sigmoid(jnp.einsum('sthc,shcd->sthd', conv_heads, input_gate_w.astype(jnp.float32)).reshape(2, STREAM_ITEMS, W))
    decay_rate = jax.nn.softplus(-decay_param)[:, None, :]
    log_decay = -RATE_SCALE * rate_gate * decay_rate + decay_jump
    decay_factors = jnp.exp(log_decay)
    squared = jnp.exp(2.0 * log_decay)
    norm_factor = jnp.sqrt(STATE_FLOOR - jnp.expm1(2.0 * log_decay))
    drive_term = input_gate * conv_full
    states = decay_factors * prior_state + norm_factor * drive_term
    summed_states = states[0] + states[1]
    gelu_value, gelu_slope = gelu_parts(branch_gate.astype(jnp.float32))
    mixed_b = (summed_states * gelu_value).astype(jnp.bfloat16)
    branch_gate_grad = (branch_grad * summed_states * gelu_slope).astype(jnp.bfloat16)
    state_grad = branch_grad * gelu_value
    adjoint = jnp.stack([adjoint_chain(decay_factors[0], state_grad, True), adjoint_chain(decay_factors[1], state_grad, False)])
    decay_grad = adjoint * (decay_factors * prior_state - drive_term * squared / norm_factor)
    drive_grad = adjoint * norm_factor
    rate_pre = (decay_grad * (-RATE_SCALE * decay_rate) * rate_gate * (1.0 - rate_gate)).astype(jnp.bfloat16)
    input_pre = (drive_grad * conv_full * input_gate * (1.0 - input_gate)).astype(jnp.bfloat16)
    conv_grad = drive_grad * input_gate
    conv_grad = conv_grad + jnp.einsum('sthd,shcd->sthc', rate_pre.astype(jnp.float32).reshape(2, STREAM_ITEMS, HEADS, HEAD), rate_gate_w.astype(jnp.float32)).reshape(2, STREAM_ITEMS, W)
    conv_grad = conv_grad + jnp.einsum('sthd,shcd->sthc', input_pre.astype(jnp.float32).reshape(2, STREAM_ITEMS, HEADS, HEAD), input_gate_w.astype(jnp.float32)).reshape(2, STREAM_ITEMS, W)
    reach = TAPS - 1
    padded = jnp.pad(conv_grad, ((0, 0), (reach, reach), (0, 0)))
    taps_full = conv_taps.astype(jnp.float32)
    input_grad = jnp.zeros((STREAM_ITEMS, W), jnp.float32)
    for tap_index in range(TAPS):
        upper = 2 * reach - tap_index
        input_grad = input_grad + taps_full[0, tap_index] * padded[0, upper:upper + STREAM_ITEMS] + taps_full[1, tap_index] * padded[1, tap_index:tap_index + STREAM_ITEMS]
    proj_grad_t = jnp.dot(mid_grad_b.T, mixed_b, preferred_element_type=jnp.float32)
    return (gate_grads, up_grads, down_grads, proj_grad_t, input_grad.astype(jnp.bfloat16), branch_gate_grad)
```

```python
import functools

import jax
import jax.numpy as jnp
from jax import lax
from jax.experimental import pallas as pl
from jax.experimental.pallas import tpu as pltpu
from jax.sharding import PartitionSpec as P

MESH = pl.DeviceIdType.MESH

RATE_SCALE = 8.0
CLAMP_LIMIT = 7.0
SHARPNESS = 1.702
NORM_EPSILON = 1e-06
STATE_FLOOR = 0.001
GELU_CUBIC = 0.044715
GELU_SCALE = 0.7978845608028654


def gelu_parts(values):
    inside = GELU_SCALE * (values + GELU_CUBIC * values * values * values)
    tangent = jnp.tanh(inside)
    result = 0.5 * values * (1.0 + tangent)
    slope_value = 0.5 * (1.0 + tangent) + 0.5 * values * (1.0 - tangent * tangent) * GELU_SCALE * (
        1.0 + 3.0 * GELU_CUBIC * values * values
    )
    return (result, slope_value)


def greet(n, g):
    me, t = lax.axis_index("sp"), lax.axis_index("tp")
    barrier = pltpu.get_barrier_semaphore()

    def over_sp(k, carry):
        peer = lax.rem(me + k, n)
        pl.semaphore_signal(barrier, inc=1, device_id={"sp": peer}, device_id_type=MESH)
        return carry

    def over_tp(k, carry):
        peer = lax.rem(t + k, g)
        pl.semaphore_signal(barrier, inc=1, device_id={"tp": peer}, device_id_type=MESH)
        return carry

    lax.fori_loop(1, n, over_sp, 0)
    lax.fori_loop(1, g, over_tp, 0)
    pl.semaphore_wait(barrier, n + g - 2)


def remote(src, dst, send_sem, recv_sem, axis, peer):
    return pltpu.make_async_remote_copy(
        src_ref=src, dst_ref=dst, send_sem=send_sem, recv_sem=recv_sem,
        device_id={axis: peer}, device_id_type=MESH,
    )


def front_kernel(n, g, send, got, sp_send, sp_recv, tp_send, tp_recv, own_sem):
    me, t = lax.axis_index("sp"), lax.axis_index("tp")
    low = lax.rem(t, 2)
    high = t // 2
    highs = g // 2
    partner = high * 2 + 1 - low
    width = send.shape[-1]

    def block(p, q):
        return got.at[:, p, :, pl.ds(pl.multiple_of(q * width, width), width)]

    def over_sp(p):
        return remote(send.at[:, p], block(me, t), sp_send.at[p], sp_recv.at[me], "sp", p)

    def from_sp(p):
        return remote(send.at[:, p], block(p, t), sp_send.at[p], sp_recv.at[p], "sp", p)

    def over_tp(kind, p, q, peer):
        return remote(block(p, q), block(p, q), tp_send.at[kind, p], tp_recv.at[q, p], "tp", peer)

    own = pltpu.make_async_copy(send.at[:, me], block(me, t), own_sem)
    own.start()
    greet(n, g)

    def start(k, carry):
        over_sp(lax.rem(me + k, n)).start()
        return carry

    lax.fori_loop(1, n, start, 0)
    own.wait()

    def spread(p):
        for j in range(1, highs):
            over_tp(j, p, t, lax.rem(high + j, highs) * 2 + low).start()
        over_tp(0, p, t, partner).start()

    def forward(p):
        for j in range(1, highs):
            q = lax.rem(high + highs - j, highs) * 2 + low
            over_tp(j, p, q, q).wait_recv()
            over_tp(highs - 1 + j, p, q, partner).start()

    spread(me)

    def step(k, carry):
        p = lax.rem(me + n - k, n)
        from_sp(p).wait_recv()
        spread(p)
        forward(lax.rem(p + 1, n))
        return carry

    lax.fori_loop(1, n, step, 0)
    forward(lax.rem(me + 1, n))

    def finish(k, carry):
        p = lax.rem(me + n - k, n)
        for j in range(highs):
            q = lax.rem(high + highs - j, highs) * 2 + 1 - low
            over_tp(0, p, q, partner).wait_recv()
        for kind in range(2 * highs - 1):
            over_tp(kind, p, t, partner).wait_send()
        return carry

    lax.fori_loop(0, n, finish, 0)

    def sent(k, carry):
        over_sp(lax.rem(me + k, n)).wait_send()
        return carry

    lax.fori_loop(1, n, sent, 0)


def shifted(x, by, fill, down):
    rows = x.shape[0]
    at = lax.broadcasted_iota(jnp.int32, x.shape, 0)
    if down:
        return jnp.where(at >= by, pltpu.roll(x, by, 0), fill)
    return jnp.where(at < rows - by, pltpu.roll(x, rows - by, 0), fill)


def chain_scan(factors, seeds, down):
    by = 1
    while by < seeds.shape[0]:
        seeds = seeds + factors * shifted(seeds, by, 0.0, down)
        factors = factors * shifted(factors, by, 1.0, down)
        by *= 2
    return factors, seeds


def dot_last(a, b):
    return lax.dot_general(a, b, (((1,), (1,)), ((), ())), preferred_element_type=jnp.float32)


def back_kernel(
    n, g, partial, select, mid, out_grad, out_proj, branch_gate, conv, prior, rate_w, input_w,
    rate, jump, taps, proj_o, input_o, branch_o,
    pair, held, crossed, ready, returned, total, token, midg, decay, rate_c, input_c, drive_c,
    proj, proj_send, proj_recv, carry_send, carries, padded,
    pair_send, pair_recv, high_send, high_recv, sp_send, sp_recv, tok_send, tok_recv,
    rs_send, rs_recv, map_send, map_recv, halo_send, halo_recv,
):
    me, t = lax.axis_index("sp"), lax.axis_index("tp")
    low = lax.rem(t, 2)
    high = t // 2
    highs = g // 2
    partner = high * 2 + 1 - low
    width = returned.shape[-1]
    rows, channels = branch_gate.shape
    f32 = jnp.float32

    def cols(q):
        return pl.ds(pl.multiple_of(q * width, width), width)

    def to_pair(h, p):
        return remote(
            partial.at[p, :, cols(h * 2 + 1 - low)], pair.at[h, p],
            pair_send.at[h, p], pair_recv.at[h, p], "tp", partner,
        )

    def to_high(j, p):
        return remote(
            held.at[j - 1, p], crossed.at[j - 1, p],
            high_send.at[j - 1, p], high_recv.at[j - 1, p], "tp",
            lax.rem(high + j, highs) * 2 + low,
        )

    def to_sp(p):
        return remote(ready.at[p], returned.at[me], sp_send.at[p], sp_recv.at[me], "sp", p)

    def from_sp(p):
        return remote(ready.at[p], returned.at[p], sp_send.at[p], sp_recv.at[p], "sp", p)

    greet(n, g)

    def first(k, carry):
        p = lax.rem(me + k, n)
        for j in range(1, highs + 1):
            to_pair(lax.rem(high + j, highs), p).start()
        return carry

    lax.fori_loop(1, n + 1, first, 0)

    def second(k, carry):
        p = lax.rem(me + k, n)
        for j in range(1, highs):
            h = lax.rem(high + j, highs)
            to_pair(h, p).wait_recv()
            held[j - 1, p] = (
                partial[p, :, cols(h * 2 + low)].astype(f32) + pair[h, p].astype(f32)
            ).astype(jnp.bfloat16)
            to_high(j, p).start()
        return carry

    lax.fori_loop(1, n + 1, second, 0)

    summed = jnp.zeros((rows, channels), f32)
    for side in range(2):
        taken = conv[side]
        rate_gate = jax.nn.sigmoid(jnp.dot(taken, rate_w[side], preferred_element_type=f32))
        input_gate = jax.nn.sigmoid(jnp.dot(taken, input_w[side], preferred_element_type=f32))
        speed = rate[side : side + 1, :]
        log_decay = speed * rate_gate + jump[side]
        factors = jnp.exp(log_decay)
        squared = jnp.exp(2.0 * log_decay)
        norm_factor = jnp.sqrt((1.0 + STATE_FLOOR) - squared)
        full = taken.astype(f32)
        drive = input_gate * full
        carried = factors * prior[side]
        summed = summed + carried + norm_factor * drive
        decay[side] = factors
        rate_c[side] = (
            (carried - drive * squared / norm_factor) * speed * rate_gate * (1.0 - rate_gate)
        )
        input_c[side] = norm_factor * full * input_gate * (1.0 - input_gate)
        drive_c[side] = norm_factor * input_gate
    gelu_value, gelu_slope = gelu_parts(branch_gate[...].astype(f32))
    mixed = (summed * gelu_value).astype(jnp.bfloat16)
    slope = summed * gelu_slope

    def third(k, carry):
        p = lax.rem(me + k, n)
        to_pair(high, p).wait_recv()
        value = partial[p, :, cols(t)].astype(f32) + pair[high, p].astype(f32)
        for j in range(1, highs):
            to_high(j, p).wait_recv()
            value = value + crossed[j - 1, p].astype(f32)
        ready[p] = value.astype(jnp.bfloat16)

        @pl.when(k < n)
        def _():
            to_sp(p).start()

        return carry

    lax.fori_loop(1, n + 1, third, 0)
    total[...] = jnp.dot(select[me], ready[me], preferred_element_type=f32)

    def fourth(k, carry):
        p = lax.rem(me + n - k, n)
        from_sp(p).wait_recv()
        total[...] += jnp.dot(select[p], returned[p], preferred_element_type=f32)
        return carry

    lax.fori_loop(1, n, fourth, 0)

    def share(kind, q, peer):
        return remote(
            token.at[:, cols(q)], token.at[:, cols(q)], tok_send.at[kind], tok_recv.at[q],
            "tp", peer,
        )

    token[:, cols(t)] = total[...].astype(jnp.bfloat16)
    for j in range(1, highs):
        share(j, t, lax.rem(high + j, highs) * 2 + low).start()
    share(0, t, partner).start()
    for j in range(1, highs):
        q = lax.rem(high + highs - j, highs) * 2 + low
        share(j, q, q).wait_recv()
        share(highs - 1 + j, q, partner).start()
    for j in range(highs):
        q = lax.rem(high + highs - j, highs) * 2 + 1 - low
        share(0, q, partner).wait_recv()

    piece = 16

    def normal(k, carry):
        at = pl.ds(pl.multiple_of(k * piece, piece), piece)
        values = mid[at, :].astype(f32)
        inv_rms = lax.rsqrt(jnp.mean(values * values, axis=1, keepdims=True) + NORM_EPSILON)
        normed = values * inv_rms
        grad = token[at, :].astype(f32)
        inner = jnp.mean(grad * normed, axis=1, keepdims=True)
        midg[at, :] = (
            out_grad[at, :].astype(f32) + inv_rms * (grad - normed * inner)
        ).astype(jnp.bfloat16)
        return carry

    lax.fori_loop(0, rows // piece, normal, 0)

    branch_grad = dot_last(midg[...], out_proj[...])
    branch_o[...] = (branch_grad * slope).astype(jnp.bfloat16)
    seeds = branch_grad * gelu_value
    later_prod, later_local = chain_scan(shifted(decay[0], 1, 1.0, False), seeds, False)
    earlier_prod, earlier_local = chain_scan(shifted(decay[1], 1, 1.0, True), seeds, True)
    first_decay, last_decay = decay[0, 0:1, :], decay[1, rows - 1 : rows, :]
    carry_send[0:1, :] = first_decay * later_prod[0:1]
    carry_send[1:2, :] = first_decay * later_local[0:1]
    carry_send[2:3, :] = last_decay * earlier_prod[rows - 1 : rows]
    carry_send[3:4, :] = last_decay * earlier_local[rows - 1 : rows]
    carry_send[4:8, :] = jnp.zeros((4, channels), f32)

    def to_map(p):
        return remote(carry_send, carries.at[me], map_send.at[p], map_recv.at[me], "sp", p)

    def from_map(p):
        return remote(carry_send, carries.at[p], map_send.at[p], map_recv.at[p], "sp", p)

    def maps(k, carry):
        to_map(lax.rem(me + k, n)).start()
        return carry

    lax.fori_loop(1, n, maps, 0)
    carries[me] = carry_send[...]

    product = lax.dot_general(
        midg[...], mixed, (((0,), (0,)), ((), ())), preferred_element_type=f32
    ).reshape(proj.shape)
    proj[...] = product
    proj_send[...] = product.astype(jnp.bfloat16)

    def to_rs(p):
        return remote(proj_send.at[p], proj_recv.at[me], rs_send.at[p], rs_recv.at[me], "sp", p)

    def from_rs(p):
        return remote(proj_send.at[p], proj_recv.at[p], rs_send.at[p], rs_recv.at[p], "sp", p)

    def scatter(k, carry):
        to_rs(lax.rem(me + k, n)).start()
        return carry

    lax.fori_loop(1, n, scatter, 0)

    def landed(k, carry):
        from_map(lax.rem(me + n - k, n)).wait_recv()
        return carry

    lax.fori_loop(1, n, landed, 0)

    def flow(k, carry):
        later, earlier = carry
        j = n - 1 - k
        later = jnp.where(j > me, carries[j, 0:1, :] * later + carries[j, 1:2, :], later)
        earlier = jnp.where(k < me, carries[k, 2:3, :] * earlier + carries[k, 3:4, :], earlier)
        return later, earlier

    nothing = jnp.zeros((1, channels), f32)
    later_in, earlier_in = lax.fori_loop(0, n, flow, (nothing, nothing))
    adjoints = (later_local + later_prod * later_in, earlier_local + earlier_prod * earlier_in)
    edge = 8
    for side in range(2):
        adjoint = adjoints[side]
        rate_pre = (adjoint * rate_c[side]).astype(jnp.bfloat16)
        input_pre = (adjoint * input_c[side]).astype(jnp.bfloat16)
        padded[side, edge : edge + rows, :] = (
            adjoint * drive_c[side]
            + dot_last(rate_pre, rate_w[side])
            + dot_last(input_pre, input_w[side])
        )
    after, before = lax.rem(me + 1, n), lax.rem(me + n - 1, n)
    up = remote(
        padded.at[:, pl.ds(rows, edge)], padded.at[:, pl.ds(0, edge)],
        halo_send.at[0], halo_recv.at[0], "sp", after,
    )
    down = remote(
        padded.at[:, pl.ds(edge, edge)], padded.at[:, pl.ds(edge + rows, edge)],
        halo_send.at[1], halo_recv.at[1], "sp", before,
    )
    up.start()
    down.start()
    up.wait()
    down.wait()
    reach = taps.shape[1] - 1
    front = jnp.where(me > 0, padded[:, 0:edge, :], 0.0)
    end = jnp.where(me < n - 1, padded[:, edge + rows : 2 * edge + rows, :], 0.0)
    padded[:, 0:edge, :] = front
    padded[:, edge + rows : 2 * edge + rows, :] = end
    result = jnp.zeros((rows, channels), f32)
    for k in range(reach + 1):
        result = (
            result
            + taps[0, k : k + 1, :] * padded[0, edge + reach - k : edge + reach - k + rows, :]
            + taps[1, k : k + 1, :] * padded[1, edge - reach + k : edge - reach + k + rows, :]
        )
    input_o[...] = result.astype(jnp.bfloat16)

    proj_o[...] = proj[me]

    def gather(k, carry):
        p = lax.rem(me + n - k, n)
        from_rs(p).wait_recv()
        proj_o[...] += proj_recv[p].astype(f32)
        return carry

    lax.fori_loop(1, n, gather, 0)

    def sent(k, carry):
        p = lax.rem(me + k, n)
        to_sp(p).wait_send()
        to_map(p).wait_send()
        to_rs(p).wait_send()
        return carry

    lax.fori_loop(1, n, sent, 0)

    def sent_tp(p, carry):
        for h in range(highs):
            to_pair(h, p).wait_send()
        for j in range(1, highs):
            to_high(j, p).wait_send()
        return carry

    lax.fori_loop(0, n, sent_tp, 0)
    for kind in range(2 * highs - 1):
        share(kind, t, partner).wait_send()


def on_device(
    mid,
    out_grad,
    expert_ids,
    route_weights,
    gate_proj,
    up_proj,
    down_proj,
    out_proj,
    branch_gate,
    conv_out,
    prior_state,
    rate_gate_w,
    input_gate_w,
    decay_param,
    decay_jump,
    conv_taps,
):
    tok_rows, embedding_width = mid.shape
    shards = lax.axis_size("sp")
    groups = lax.axis_size("tp")
    local_experts = gate_proj.shape[0]
    experts_all = local_experts * shards
    top_count = expert_ids.shape[1]
    expert_room = 3 * top_count * tok_rows // (2 * experts_all)
    slot_count = experts_all * expert_room
    mid_full = mid.astype(jnp.float32)
    inv_rms = lax.rsqrt(jnp.mean(mid_full * mid_full, axis=1, keepdims=True) + NORM_EPSILON)
    normed = mid_full * inv_rms
    normed_b = normed.astype(jnp.bfloat16)
    flat_ids = expert_ids.reshape(-1)
    onehot = (flat_ids[:, None] == jnp.arange(experts_all, dtype=jnp.int32)[None, :]).astype(
        jnp.int32
    )
    rank_ids = jnp.sum((jnp.cumsum(onehot, axis=0) - onehot) * onehot, axis=1)
    slot_ids = (flat_ids * expert_room + rank_ids).reshape(tok_rows, top_count)
    matches = slot_ids[None, :, :] == jnp.arange(slot_count, dtype=jnp.int32)[:, None, None]
    select = jnp.any(matches, axis=2).astype(jnp.bfloat16)
    slot_gate = jnp.sum(jnp.where(matches, route_weights[None, :, :], 0.0), axis=(1, 2))
    column_span = embedding_width // groups
    offset = lax.axis_index("tp") * column_span
    rows_source = lax.dynamic_slice_in_dim(normed_b, offset, column_span, 1)
    grad_source = lax.dynamic_slice_in_dim(out_grad, offset, column_span, 1)
    sent_rows = jnp.dot(select, rows_source, preferred_element_type=jnp.float32).astype(
        jnp.bfloat16
    )
    dispatched_cotangent = (
        jnp.dot(select, grad_source, preferred_element_type=jnp.float32) * slot_gate[:, None]
    ).astype(jnp.bfloat16)
    sending = jnp.stack([sent_rows, dispatched_cotangent]).reshape(
        2, shards, local_experts * expert_room, column_span
    )
    dma = pltpu.SemaphoreType.DMA
    vmem = pl.BlockSpec(memory_space=pltpu.VMEM)
    got = pl.pallas_call(
        functools.partial(front_kernel, shards, groups),
        out_shape=jax.ShapeDtypeStruct(
            (2, shards, local_experts * expert_room, embedding_width), jnp.bfloat16
        ),
        in_specs=[vmem],
        out_specs=vmem,
        scratch_shapes=[
            dma((shards,)), dma((shards,)), dma((groups - 1, shards)), dma((groups, shards)),
            dma(()),
        ],
        compiler_params=pltpu.CompilerParams(collective_id=0, has_side_effects=True),
    )(sending)

    def by_expert(block):
        return jnp.swapaxes(
            block.reshape(shards, local_experts, expert_room, embedding_width), 0, 1
        ).reshape(local_experts, shards * expert_room, embedding_width)

    expert_rows, expert_grads = by_expert(got[0]), by_expert(got[1])
    gate_pre = jnp.einsum(
        "erd,edf->erf", expert_rows, gate_proj, preferred_element_type=jnp.float32
    )
    up_pre = jnp.einsum("erd,edf->erf", expert_rows, up_proj, preferred_element_type=jnp.float32)
    gate_clamped = jnp.minimum(gate_pre, CLAMP_LIMIT)
    up_clamped = jnp.clip(up_pre, -CLAMP_LIMIT, CLAMP_LIMIT)
    gate_sigmoid = jax.nn.sigmoid(SHARPNESS * gate_clamped)
    swish_value = gate_clamped * gate_sigmoid
    act_b = ((up_clamped + 1.0) * swish_value).astype(jnp.bfloat16)
    act_grad = jnp.einsum(
        "erd,efd->erf", expert_grads, down_proj, preferred_element_type=jnp.float32
    )
    gate_delta = jnp.where(
        gate_pre < CLAMP_LIMIT,
        act_grad
        * (up_clamped + 1.0)
        * (gate_sigmoid + SHARPNESS * swish_value * (1.0 - gate_sigmoid)),
        0.0,
    ).astype(jnp.bfloat16)
    up_delta = jnp.where(jnp.abs(up_pre) < CLAMP_LIMIT, act_grad * swish_value, 0.0).astype(
        jnp.bfloat16
    )
    down_grad = jnp.einsum(
        "erf,erd->efd", act_b, expert_grads, preferred_element_type=jnp.float32
    ).astype(jnp.bfloat16)
    gate_grad = jnp.einsum(
        "erd,erf->edf", expert_rows, gate_delta, preferred_element_type=jnp.float32
    ).astype(jnp.bfloat16)
    up_grad = jnp.einsum(
        "erd,erf->edf", expert_rows, up_delta, preferred_element_type=jnp.float32
    ).astype(jnp.bfloat16)
    partial_value = jnp.einsum(
        "erf,edf->erd", gate_delta, gate_proj, preferred_element_type=jnp.float32
    )
    partial_value = partial_value + jnp.einsum(
        "erf,edf->erd", up_delta, up_proj, preferred_element_type=jnp.float32
    )
    room = local_experts * expert_room
    partial_rows = jnp.swapaxes(
        partial_value.reshape(local_experts, shards, expert_room, embedding_width), 0, 1
    ).reshape(shards, room, embedding_width).astype(jnp.bfloat16)
    token_slots = jnp.arange(slot_count, dtype=jnp.int32).reshape(shards, 1, room)
    select_t = jnp.any(
        slot_ids[None, :, None, :] == token_slots[:, :, :, None], axis=3
    ).astype(jnp.bfloat16)
    heads_local = rate_gate_w.shape[1]
    head_width = rate_gate_w.shape[2]
    channels = heads_local * head_width
    same_head = jnp.eye(heads_local, dtype=jnp.bfloat16)[None, :, None, :, None]

    def block_diagonal(blocks):
        return (blocks[:, :, :, None, :] * same_head).reshape(2, channels, channels)

    speed = -RATE_SCALE * jax.nn.softplus(-decay_param)
    highs = groups // 2
    bf16, f32 = jnp.bfloat16, jnp.float32
    proj_rows = embedding_width // shards
    proj_grad_t, input_grad, branch_gate_grad = pl.pallas_call(
        functools.partial(back_kernel, shards, groups),
        out_shape=(
            jax.ShapeDtypeStruct((proj_rows, channels), f32),
            jax.ShapeDtypeStruct((tok_rows, channels), bf16),
            jax.ShapeDtypeStruct((tok_rows, channels), bf16),
        ),
        in_specs=[vmem] * 13,
        out_specs=(vmem,) * 3,
        scratch_shapes=[
            pltpu.VMEM((highs, shards, room, column_span), bf16),
            pltpu.VMEM((highs - 1, shards, room, column_span), bf16),
            pltpu.VMEM((highs - 1, shards, room, column_span), bf16),
            pltpu.VMEM((shards, room, column_span), bf16),
            pltpu.VMEM((shards, room, column_span), bf16),
            pltpu.VMEM((tok_rows, column_span), f32),
            pltpu.VMEM((tok_rows, embedding_width), bf16),
            pltpu.VMEM((tok_rows, embedding_width), bf16),
            pltpu.VMEM((2, tok_rows, channels), f32),
            pltpu.VMEM((2, tok_rows, channels), f32),
            pltpu.VMEM((2, tok_rows, channels), f32),
            pltpu.VMEM((2, tok_rows, channels), f32),
            pltpu.VMEM((shards, proj_rows, channels), f32),
            pltpu.VMEM((shards, proj_rows, channels), bf16),
            pltpu.VMEM((shards, proj_rows, channels), bf16),
            pltpu.VMEM((8, channels), f32),
            pltpu.VMEM((shards, 8, channels), f32),
            pltpu.VMEM((2, tok_rows + 16, channels), f32),
            dma((highs, shards)), dma((highs, shards)),
            dma((highs - 1, shards)), dma((highs - 1, shards)),
            dma((shards,)), dma((shards,)),
            dma((groups - 1,)), dma((groups,)),
            dma((shards,)), dma((shards,)),
            dma((shards,)), dma((shards,)),
            dma((2,)), dma((2,)),
        ],
        compiler_params=pltpu.CompilerParams(collective_id=1, has_side_effects=True),
    )(
        partial_rows, select_t, mid, out_grad, out_proj, branch_gate, conv_out, prior_state,
        block_diagonal(rate_gate_w), block_diagonal(input_gate_w), speed, decay_jump,
        conv_taps.astype(f32),
    )
    return (gate_grad, up_grad, down_grad, proj_grad_t, input_grad, branch_gate_grad)


def solution(mesh):
    in_specs = (
        P("sp", None),
        P("sp", None),
        P("sp", None),
        P("sp", None),
        P("sp", None, "tp"),
        P("sp", None, "tp"),
        P("sp", "tp", None),
        P("tp", None),
        P("sp", "tp"),
        P(None, "sp", "tp"),
        P(None, "sp", "tp"),
        P(None, "tp", None, None),
        P(None, "tp", None, None),
        P(None, "tp"),
        P(None, "sp", "tp"),
        P(None, None, "tp"),
    )
    out_specs = (
        P("sp", None, "tp"),
        P("sp", None, "tp"),
        P("sp", "tp", None),
        P("sp", "tp"),
        P("sp", "tp"),
        P("sp", "tp"),
    )
    return jax.shard_map(
        on_device, mesh=mesh, in_specs=in_specs, out_specs=out_specs, check_vma=False
    )
```

```python
import functools

import jax
import jax.numpy as jnp
from jax import lax
from jax.experimental import pallas as pl
from jax.experimental.pallas import tpu as pltpu
from jax.sharding import PartitionSpec as P

MESH = pl.DeviceIdType.MESH

RATE_SCALE = 8.0
CLAMP_LIMIT = 7.0
SHARPNESS = 1.702
NORM_EPSILON = 1e-06
STATE_FLOOR = 0.001
GELU_CUBIC = 0.044715
GELU_SCALE = 0.7978845608028654


def gelu_parts(values):
    inside = GELU_SCALE * (values + GELU_CUBIC * values * values * values)
    tangent = jnp.tanh(inside)
    result = 0.5 * values * (1.0 + tangent)
    slope_value = 0.5 * (1.0 + tangent) + 0.5 * values * (1.0 - tangent * tangent) * GELU_SCALE * (
        1.0 + 3.0 * GELU_CUBIC * values * values
    )
    return (result, slope_value)


def greet(n, g):
    me, t = lax.axis_index("sp"), lax.axis_index("tp")
    barrier = pltpu.get_barrier_semaphore()

    def over_sp(k, carry):
        peer = lax.rem(me + k, n)
        pl.semaphore_signal(barrier, inc=1, device_id={"sp": peer}, device_id_type=MESH)
        return carry

    def over_tp(k, carry):
        peer = lax.rem(t + k, g)
        pl.semaphore_signal(barrier, inc=1, device_id={"tp": peer}, device_id_type=MESH)
        return carry

    lax.fori_loop(1, n, over_sp, 0)
    lax.fori_loop(1, g, over_tp, 0)


def greeted(n, g):
    pl.semaphore_wait(pltpu.get_barrier_semaphore(), n + g - 2)


def remote(src, dst, send_sem, recv_sem, axis, peer):
    return pltpu.make_async_remote_copy(
        src_ref=src, dst_ref=dst, send_sem=send_sem, recv_sem=recv_sem,
        device_id={axis: peer}, device_id_type=MESH,
    )


def front_kernel(
    n, g, mid, out_grad, ids, weights, got_rows, got_grads, select, send, normed, ahead, named, gains,
    sp_send, sp_recv, tp_send, tp_recv,
):
    me, t = lax.axis_index("sp"), lax.axis_index("tp")
    low = lax.rem(t, 2)
    high = t // 2
    highs = g // 2
    partner = high * 2 + 1 - low
    width = send.shape[-1]

    both = (got_rows, got_grads)

    def block(a, p, q):
        return both[a].at[p, :, pl.ds(pl.multiple_of(q * width, width), width)]

    def over_sp(a, p):
        return remote(
            send.at[a, p], block(a, me, t), sp_send.at[a, p], sp_recv.at[a, me], "sp", p
        )

    def from_sp(a, p):
        return remote(
            send.at[a, p], block(a, p, t), sp_send.at[a, p], sp_recv.at[a, p], "sp", p
        )

    def over_tp(a, kind, p, q, peer):
        return remote(
            block(a, p, q), block(a, p, q), tp_send.at[a, kind, p], tp_recv.at[a, q, p], "tp", peer
        )

    greet(n, g)
    rows = mid.shape[0]
    experts, top = named.shape[0], ids.shape[0]
    per = experts // n
    room = select.shape[1] // per
    f32, bf16 = jnp.float32, jnp.bfloat16
    mine = pl.ds(pl.multiple_of(t * width, width), width)
    piece = 16

    def normal(k, carry):
        at = pl.ds(pl.multiple_of(k * piece, piece), piece)
        values = mid[at, :].astype(f32)
        inv_rms = lax.rsqrt(jnp.mean(values * values, axis=1, keepdims=True) + NORM_EPSILON)
        normed[at, :] = (mid[at, mine].astype(f32) * inv_rms).astype(bf16)
        return carry

    lax.fori_loop(0, rows // piece, normal, 0)
    number = lax.broadcasted_iota(jnp.int32, (experts, rows), 0)
    hit = jnp.zeros((experts, rows), f32)
    gain = jnp.zeros((experts, rows), f32)
    for k in range(top):
        here = ids[k : k + 1, :] == number
        hit = hit + jnp.where(here, 1.0, 0.0)
        gain = gain + jnp.where(here, weights[k : k + 1, :], 0.0)
    before = lax.broadcasted_iota(jnp.int32, (rows, rows), 0) < lax.broadcasted_iota(
        jnp.int32, (rows, rows), 1
    )
    ahead[...] = jnp.dot(
        hit.astype(bf16), jnp.where(before, 1.0, 0.0).astype(bf16), preferred_element_type=f32
    )
    named[...] = hit
    gains[...] = gain
    place = lax.broadcasted_iota(jnp.int32, (room, rows), 0).astype(f32)

    def build(p):
        picks, scales = [], []
        for j in range(per):
            e = p * per + j
            pick = jnp.where(
                (ahead[pl.ds(e, 1), :] == place) & (named[pl.ds(e, 1), :] > 0.5), 1.0, 0.0
            )
            picks.append(pick)
            scales.append(jnp.sum(pick * gains[pl.ds(e, 1), :], axis=1, keepdims=True))
        pick = picks[0] if per == 1 else jnp.concatenate(picks, axis=0)
        scale = scales[0] if per == 1 else jnp.concatenate(scales, axis=0)
        pick = pick.astype(bf16)
        select[p] = pick
        sent = jnp.dot(pick, normed[...], preferred_element_type=f32).astype(bf16)
        grads = jnp.dot(pick, out_grad[:, mine], preferred_element_type=f32) * scale
        return sent, grads.astype(bf16)

    def spread(a, p):
        for j in range(1, highs):
            over_tp(a, j, p, t, lax.rem(high + j, highs) * 2 + low).start()
        over_tp(a, 0, p, t, partner).start()

    def forward(a, p):
        for j in range(1, highs):
            q = lax.rem(high + highs - j, highs) * 2 + low
            over_tp(a, j, p, q, q).wait_recv()
            over_tp(a, highs - 1 + j, p, q, partner).start()

    own_rows, own_grads = build(me)
    got_rows[me, :, mine] = own_rows
    got_grads[me, :, mine] = own_grads
    greeted(n, g)
    for a in range(2):
        spread(a, me)

    def start(k, carry):
        p = lax.rem(me + k, n)
        send[0, p], send[1, p] = build(p)
        for a in range(2):
            over_sp(a, p).start()
        return carry

    lax.fori_loop(1, n, start, 0)

    def step(k, carry):
        p = lax.rem(me + n - k, n)
        for a in range(2):
            from_sp(a, p).wait_recv()
            spread(a, p)
        for a in range(2):
            forward(a, lax.rem(p + 1, n))
        return carry

    lax.fori_loop(1, n, step, 0)
    for a in range(2):
        forward(a, lax.rem(me + 1, n))

    def finish(k, carry):
        p = lax.rem(me + n - k, n)
        for a in range(2):
            for j in range(highs):
                q = lax.rem(high + highs - j, highs) * 2 + 1 - low
                over_tp(a, 0, p, q, partner).wait_recv()
            for kind in range(2 * highs - 1):
                over_tp(a, kind, p, t, partner).wait_send()
        return carry

    lax.fori_loop(0, n, finish, 0)

    def sent(k, carry):
        for a in range(2):
            over_sp(a, lax.rem(me + k, n)).wait_send()
        return carry

    lax.fori_loop(1, n, sent, 0)


def shifted(x, by, fill, down):
    rows = x.shape[0]
    at = lax.broadcasted_iota(jnp.int32, x.shape, 0)
    if down:
        return jnp.where(at >= by, pltpu.roll(x, by, 0), fill)
    return jnp.where(at < rows - by, pltpu.roll(x, rows - by, 0), fill)


def chain_scan(factors, seeds, down):
    by = 1
    while by < seeds.shape[0]:
        seeds = seeds + factors * shifted(seeds, by, 0.0, down)
        factors = factors * shifted(factors, by, 1.0, down)
        by *= 2
    return factors, seeds


def dot_last(a, b):
    return lax.dot_general(a, b, (((1,), (1,)), ((), ())), preferred_element_type=jnp.float32)


def dot_first(a, b):
    return lax.dot_general(a, b, (((0,), (0,)), ((), ())), preferred_element_type=jnp.float32)


def hand_on(a, b, c, x, y, z):
    x[...] = a[...]
    y[...] = b[...]
    z[...] = c[...]


def back_kernel(
    n, g, partial, select, mid, out_grad, out_proj, branch_gate, conv, prior, rate_w, input_w,
    rate, jump, taps, proj_o, input_o, branch_o,
    pair, held, crossed, ready, returned, total, token, midg, decay, rate_c, input_c, drive_c,
    proj, proj_send, proj_recv, carry_send, carries, padded,
    pair_send, pair_recv, high_send, high_recv, sp_send, sp_recv, tok_send, tok_recv,
    rs_send, rs_recv, map_send, map_recv, halo_send, halo_recv,
):
    me, t = lax.axis_index("sp"), lax.axis_index("tp")
    low = lax.rem(t, 2)
    high = t // 2
    highs = g // 2
    partner = high * 2 + 1 - low
    width = returned.shape[-1]
    rows, channels = branch_gate.shape
    f32 = jnp.float32

    def cols(q):
        return pl.ds(pl.multiple_of(q * width, width), width)

    def to_pair(h, p):
        return remote(
            partial.at[p, :, cols(h * 2 + 1 - low)], pair.at[h, p],
            pair_send.at[h, p], pair_recv.at[h, p], "tp", partner,
        )

    def to_high(j, p):
        return remote(
            held.at[j - 1, p], crossed.at[j - 1, p],
            high_send.at[j - 1, p], high_recv.at[j - 1, p], "tp",
            lax.rem(high + j, highs) * 2 + low,
        )

    def to_sp(p):
        return remote(ready.at[p], returned.at[me], sp_send.at[p], sp_recv.at[me], "sp", p)

    def from_sp(p):
        return remote(ready.at[p], returned.at[p], sp_send.at[p], sp_recv.at[p], "sp", p)

    greet(n, g)
    greeted(n, g)

    def first(k, carry):
        p = lax.rem(me + k, n)
        for j in range(1, highs + 1):
            to_pair(lax.rem(high + j, highs), p).start()
        return carry

    lax.fori_loop(1, n + 1, first, 0)

    def second(k, carry):
        p = lax.rem(me + k, n)
        for j in range(1, highs):
            h = lax.rem(high + j, highs)
            to_pair(h, p).wait_recv()
            held[j - 1, p] = (
                partial[p, :, cols(h * 2 + low)].astype(f32) + pair[h, p].astype(f32)
            ).astype(jnp.bfloat16)
            to_high(j, p).start()
        return carry

    lax.fori_loop(1, n + 1, second, 0)

    summed = jnp.zeros((rows, channels), f32)
    for side in range(2):
        taken = conv[side]
        rate_gate = jax.nn.sigmoid(jnp.dot(taken, rate_w[side], preferred_element_type=f32))
        input_gate = jax.nn.sigmoid(jnp.dot(taken, input_w[side], preferred_element_type=f32))
        speed = rate[side : side + 1, :]
        log_decay = speed * rate_gate + jump[side]
        factors = jnp.exp(log_decay)
        squared = jnp.exp(2.0 * log_decay)
        norm_factor = jnp.sqrt((1.0 + STATE_FLOOR) - squared)
        full = taken.astype(f32)
        drive = input_gate * full
        carried = factors * prior[side]
        summed = summed + carried + norm_factor * drive
        decay[side] = factors
        rate_c[side] = (
            (carried - drive * squared / norm_factor) * speed * rate_gate * (1.0 - rate_gate)
        )
        input_c[side] = norm_factor * full * input_gate * (1.0 - input_gate)
        drive_c[side] = norm_factor * input_gate
    gelu_value, gelu_slope = gelu_parts(branch_gate[...].astype(f32))
    mixed = (summed * gelu_value).astype(jnp.bfloat16)
    slope = summed * gelu_slope

    def third(k, carry):
        p = lax.rem(me + k, n)
        to_pair(high, p).wait_recv()
        value = partial[p, :, cols(t)].astype(f32) + pair[high, p].astype(f32)
        for j in range(1, highs):
            to_high(j, p).wait_recv()
            value = value + crossed[j - 1, p].astype(f32)
        ready[p] = value.astype(jnp.bfloat16)

        @pl.when(k < n)
        def _():
            to_sp(p).start()

        return carry

    lax.fori_loop(1, n + 1, third, 0)
    total[...] = dot_first(select[me], ready[me])

    def fourth(k, carry):
        p = lax.rem(me + n - k, n)
        from_sp(p).wait_recv()
        total[...] += dot_first(select[p], returned[p])
        return carry

    lax.fori_loop(1, n, fourth, 0)

    def share(kind, q, peer):
        return remote(
            token.at[:, cols(q)], token.at[:, cols(q)], tok_send.at[kind], tok_recv.at[q],
            "tp", peer,
        )

    token[:, cols(t)] = total[...].astype(jnp.bfloat16)
    for j in range(1, highs):
        share(j, t, lax.rem(high + j, highs) * 2 + low).start()
    share(0, t, partner).start()
    for j in range(1, highs):
        q = lax.rem(high + highs - j, highs) * 2 + low
        share(j, q, q).wait_recv()
        share(highs - 1 + j, q, partner).start()
    for j in range(highs):
        q = lax.rem(high + highs - j, highs) * 2 + 1 - low
        share(0, q, partner).wait_recv()

    piece = 16

    def normal(k, carry):
        at = pl.ds(pl.multiple_of(k * piece, piece), piece)
        values = mid[at, :].astype(f32)
        inv_rms = lax.rsqrt(jnp.mean(values * values, axis=1, keepdims=True) + NORM_EPSILON)
        normed = values * inv_rms
        grad = token[at, :].astype(f32)
        inner = jnp.mean(grad * normed, axis=1, keepdims=True)
        midg[at, :] = (
            out_grad[at, :].astype(f32) + inv_rms * (grad - normed * inner)
        ).astype(jnp.bfloat16)
        return carry

    lax.fori_loop(0, rows // piece, normal, 0)

    branch_grad = dot_last(midg[...], out_proj[...])
    branch_o[...] = (branch_grad * slope).astype(jnp.bfloat16)
    seeds = branch_grad * gelu_value
    later_prod, later_local = chain_scan(shifted(decay[0], 1, 1.0, False), seeds, False)
    earlier_prod, earlier_local = chain_scan(shifted(decay[1], 1, 1.0, True), seeds, True)
    first_decay, last_decay = decay[0, 0:1, :], decay[1, rows - 1 : rows, :]
    carry_send[0:1, :] = first_decay * later_prod[0:1]
    carry_send[1:2, :] = first_decay * later_local[0:1]
    carry_send[2:3, :] = last_decay * earlier_prod[rows - 1 : rows]
    carry_send[3:4, :] = last_decay * earlier_local[rows - 1 : rows]
    carry_send[4:8, :] = jnp.zeros((4, channels), f32)

    def to_map(p):
        return remote(carry_send, carries.at[me], map_send.at[p], map_recv.at[me], "sp", p)

    def from_map(p):
        return remote(carry_send, carries.at[p], map_send.at[p], map_recv.at[p], "sp", p)

    def maps(k, carry):
        to_map(lax.rem(me + k, n)).start()
        return carry

    lax.fori_loop(1, n, maps, 0)
    carries[me] = carry_send[...]

    product = lax.dot_general(
        midg[...], mixed, (((0,), (0,)), ((), ())), preferred_element_type=f32
    ).reshape(proj.shape)
    proj[...] = product
    proj_send[...] = product.astype(jnp.bfloat16)

    def to_rs(p):
        return remote(proj_send.at[p], proj_recv.at[me], rs_send.at[p], rs_recv.at[me], "sp", p)

    def from_rs(p):
        return remote(proj_send.at[p], proj_recv.at[p], rs_send.at[p], rs_recv.at[p], "sp", p)

    def scatter(k, carry):
        to_rs(lax.rem(me + k, n)).start()
        return carry

    lax.fori_loop(1, n, scatter, 0)

    def landed(k, carry):
        from_map(lax.rem(me + n - k, n)).wait_recv()
        return carry

    lax.fori_loop(1, n, landed, 0)

    def flow(k, carry):
        later, earlier = carry
        j = n - 1 - k
        later = jnp.where(j > me, carries[j, 0:1, :] * later + carries[j, 1:2, :], later)
        earlier = jnp.where(k < me, carries[k, 2:3, :] * earlier + carries[k, 3:4, :], earlier)
        return later, earlier

    nothing = jnp.zeros((1, channels), f32)
    later_in, earlier_in = lax.fori_loop(0, n, flow, (nothing, nothing))
    adjoints = (later_local + later_prod * later_in, earlier_local + earlier_prod * earlier_in)
    edge = 8
    for side in range(2):
        adjoint = adjoints[side]
        rate_pre = (adjoint * rate_c[side]).astype(jnp.bfloat16)
        input_pre = (adjoint * input_c[side]).astype(jnp.bfloat16)
        padded[side, edge : edge + rows, :] = (
            adjoint * drive_c[side]
            + dot_last(rate_pre, rate_w[side])
            + dot_last(input_pre, input_w[side])
        )
    after, before = lax.rem(me + 1, n), lax.rem(me + n - 1, n)
    up = remote(
        padded.at[:, pl.ds(rows, edge)], padded.at[:, pl.ds(0, edge)],
        halo_send.at[0], halo_recv.at[0], "sp", after,
    )
    down = remote(
        padded.at[:, pl.ds(edge, edge)], padded.at[:, pl.ds(edge + rows, edge)],
        halo_send.at[1], halo_recv.at[1], "sp", before,
    )
    up.start()
    down.start()
    up.wait()
    down.wait()
    reach = taps.shape[1] - 1
    taps_full = taps[...].astype(f32)
    front = jnp.where(me > 0, padded[:, 0:edge, :], 0.0)
    end = jnp.where(me < n - 1, padded[:, edge + rows : 2 * edge + rows, :], 0.0)
    padded[:, 0:edge, :] = front
    padded[:, edge + rows : 2 * edge + rows, :] = end
    result = jnp.zeros((rows, channels), f32)
    for k in range(reach + 1):
        result = (
            result
            + taps_full[0, k : k + 1, :] * padded[0, edge + reach - k : edge + reach - k + rows, :]
            + taps_full[1, k : k + 1, :] * padded[1, edge - reach + k : edge - reach + k + rows, :]
        )
    input_o[...] = result.astype(jnp.bfloat16)

    proj_o[...] = proj[me]

    def gather(k, carry):
        p = lax.rem(me + n - k, n)
        from_rs(p).wait_recv()
        proj_o[...] += proj_recv[p].astype(f32)
        return carry

    lax.fori_loop(1, n, gather, 0)

    def sent(k, carry):
        p = lax.rem(me + k, n)
        to_sp(p).wait_send()
        to_map(p).wait_send()
        to_rs(p).wait_send()
        return carry

    lax.fori_loop(1, n, sent, 0)

    def sent_tp(p, carry):
        for h in range(highs):
            to_pair(h, p).wait_send()
        for j in range(1, highs):
            to_high(j, p).wait_send()
        return carry

    lax.fori_loop(0, n, sent_tp, 0)
    for kind in range(2 * highs - 1):
        share(kind, t, partner).wait_send()


def on_device(
    mid,
    out_grad,
    expert_ids,
    route_weights,
    gate_proj,
    up_proj,
    down_proj,
    out_proj,
    branch_gate,
    conv_out,
    prior_state,
    rate_gate_w,
    input_gate_w,
    decay_param,
    decay_jump,
    conv_taps,
):
    tok_rows, embedding_width = mid.shape
    shards = lax.axis_size("sp")
    groups = lax.axis_size("tp")
    local_experts = gate_proj.shape[0]
    experts_all = local_experts * shards
    top_count = expert_ids.shape[1]
    expert_room = 3 * top_count * tok_rows // (2 * experts_all)
    slot_count = experts_all * expert_room
    column_span = embedding_width // groups
    room = local_experts * expert_room
    dma = pltpu.SemaphoreType.DMA
    vmem = pl.BlockSpec(memory_space=pltpu.VMEM)
    got_rows, got_grads, select = pl.pallas_call(
        functools.partial(front_kernel, shards, groups),
        out_shape=(
            jax.ShapeDtypeStruct((shards, room, embedding_width), jnp.bfloat16),
            jax.ShapeDtypeStruct((shards, room, embedding_width), jnp.bfloat16),
            jax.ShapeDtypeStruct((shards, room, tok_rows), jnp.bfloat16),
        ),
        in_specs=[vmem] * 4,
        out_specs=(vmem,) * 3,
        scratch_shapes=[
            pltpu.VMEM((2, shards, room, column_span), jnp.bfloat16),
            pltpu.VMEM((tok_rows, column_span), jnp.bfloat16),
            pltpu.VMEM((experts_all, tok_rows), jnp.float32),
            pltpu.VMEM((experts_all, tok_rows), jnp.float32),
            pltpu.VMEM((experts_all, tok_rows), jnp.float32),
            dma((2, shards)), dma((2, shards)), dma((2, groups - 1, shards)),
            dma((2, groups, shards)),
        ],
        compiler_params=pltpu.CompilerParams(collective_id=0, has_side_effects=True),
    )(mid, out_grad, expert_ids.T, route_weights.T)

    def by_expert(block):
        return jnp.swapaxes(
            block.reshape(shards, local_experts, expert_room, embedding_width), 0, 1
        ).reshape(local_experts, shards * expert_room, embedding_width)

    expert_rows, expert_grads = by_expert(got_rows), by_expert(got_grads)
    gate_pre = jnp.einsum(
        "erd,edf->erf", expert_rows, gate_proj, preferred_element_type=jnp.float32
    )
    up_pre = jnp.einsum("erd,edf->erf", expert_rows, up_proj, preferred_element_type=jnp.float32)
    gate_clamped = jnp.minimum(gate_pre, CLAMP_LIMIT)
    up_clamped = jnp.clip(up_pre, -CLAMP_LIMIT, CLAMP_LIMIT)
    gate_sigmoid = jax.nn.sigmoid(SHARPNESS * gate_clamped)
    swish_value = gate_clamped * gate_sigmoid
    act_b = ((up_clamped + 1.0) * swish_value).astype(jnp.bfloat16)
    act_grad = jnp.einsum(
        "erd,efd->erf", expert_grads, down_proj, preferred_element_type=jnp.float32
    )
    gate_delta = jnp.where(
        gate_pre < CLAMP_LIMIT,
        act_grad
        * (up_clamped + 1.0)
        * (gate_sigmoid + SHARPNESS * swish_value * (1.0 - gate_sigmoid)),
        0.0,
    ).astype(jnp.bfloat16)
    up_delta = jnp.where(jnp.abs(up_pre) < CLAMP_LIMIT, act_grad * swish_value, 0.0).astype(
        jnp.bfloat16
    )
    down_grad = jnp.einsum(
        "erf,erd->efd", act_b, expert_grads, preferred_element_type=jnp.float32
    ).astype(jnp.bfloat16)
    gate_grad = jnp.einsum(
        "erd,erf->edf", expert_rows, gate_delta, preferred_element_type=jnp.float32
    ).astype(jnp.bfloat16)
    up_grad = jnp.einsum(
        "erd,erf->edf", expert_rows, up_delta, preferred_element_type=jnp.float32
    ).astype(jnp.bfloat16)
    partial_value = jnp.einsum(
        "erf,edf->erd", gate_delta, gate_proj, preferred_element_type=jnp.float32
    )
    partial_value = partial_value + jnp.einsum(
        "erf,edf->erd", up_delta, up_proj, preferred_element_type=jnp.float32
    )
    partial_rows = jnp.swapaxes(
        partial_value.reshape(local_experts, shards, expert_room, embedding_width), 0, 1
    ).reshape(shards, room, embedding_width).astype(jnp.bfloat16)
    heads_local = rate_gate_w.shape[1]
    head_width = rate_gate_w.shape[2]
    channels = heads_local * head_width
    same_head = jnp.eye(heads_local, dtype=jnp.bfloat16)[None, :, None, :, None]

    def block_diagonal(blocks):
        return (blocks[:, :, :, None, :] * same_head).reshape(2, channels, channels)

    speed = -RATE_SCALE * jax.nn.softplus(-decay_param)
    highs = groups // 2
    bf16, f32 = jnp.bfloat16, jnp.float32
    proj_rows = embedding_width // shards
    ending = pl.pallas_call(
        functools.partial(back_kernel, shards, groups),
        out_shape=(
            jax.ShapeDtypeStruct((proj_rows, channels), f32),
            jax.ShapeDtypeStruct((tok_rows, channels), bf16),
            jax.ShapeDtypeStruct((tok_rows, channels), bf16),
        ),
        in_specs=[vmem] * 13,
        out_specs=(vmem,) * 3,
        scratch_shapes=[
            pltpu.VMEM((highs, shards, room, column_span), bf16),
            pltpu.VMEM((highs - 1, shards, room, column_span), bf16),
            pltpu.VMEM((highs - 1, shards, room, column_span), bf16),
            pltpu.VMEM((shards, room, column_span), bf16),
            pltpu.VMEM((shards, room, column_span), bf16),
            pltpu.VMEM((tok_rows, column_span), f32),
            pltpu.VMEM((tok_rows, embedding_width), bf16),
            pltpu.VMEM((tok_rows, embedding_width), bf16),
            pltpu.VMEM((2, tok_rows, channels), f32),
            pltpu.VMEM((2, tok_rows, channels), f32),
            pltpu.VMEM((2, tok_rows, channels), f32),
            pltpu.VMEM((2, tok_rows, channels), f32),
            pltpu.VMEM((shards, proj_rows, channels), f32),
            pltpu.VMEM((shards, proj_rows, channels), bf16),
            pltpu.VMEM((shards, proj_rows, channels), bf16),
            pltpu.VMEM((8, channels), f32),
            pltpu.VMEM((shards, 8, channels), f32),
            pltpu.VMEM((2, tok_rows + 16, channels), f32),
            dma((highs, shards)), dma((highs, shards)),
            dma((highs - 1, shards)), dma((highs - 1, shards)),
            dma((shards,)), dma((shards,)),
            dma((groups - 1,)), dma((groups,)),
            dma((shards,)), dma((shards,)),
            dma((shards,)), dma((shards,)),
            dma((2,)), dma((2,)),
        ],
        compiler_params=pltpu.CompilerParams(collective_id=1, has_side_effects=True),
    )(
        partial_rows, select, mid, out_grad, out_proj, branch_gate, conv_out, prior_state,
        block_diagonal(rate_gate_w), block_diagonal(input_gate_w), speed, decay_jump,
        conv_taps,
    )
    proj_grad_t, input_grad, branch_gate_grad = pl.pallas_call(
        hand_on,
        out_shape=tuple(jax.ShapeDtypeStruct(x.shape, x.dtype) for x in ending),
        in_specs=[vmem] * 3,
        out_specs=(vmem,) * 3,
    )(*ending)
    return (gate_grad, up_grad, down_grad, proj_grad_t, input_grad, branch_gate_grad)


def solution(mesh):
    in_specs = (
        P("sp", None),
        P("sp", None),
        P("sp", None),
        P("sp", None),
        P("sp", None, "tp"),
        P("sp", None, "tp"),
        P("sp", "tp", None),
        P("tp", None),
        P("sp", "tp"),
        P(None, "sp", "tp"),
        P(None, "sp", "tp"),
        P(None, "tp", None, None),
        P(None, "tp", None, None),
        P(None, "tp"),
        P(None, "sp", "tp"),
        P(None, None, "tp"),
    )
    out_specs = (
        P("sp", None, "tp"),
        P("sp", None, "tp"),
        P("sp", "tp", None),
        P("sp", "tp"),
        P("sp", "tp"),
        P("sp", "tp"),
    )
    return jax.shard_map(
        on_device, mesh=mesh, in_specs=in_specs, out_specs=out_specs, check_vma=False
    )
```
